32 devices in a mesh: sp: 8 (over z, y), tp: 4 (over x, core).
Axes of the slice: x: 2, y: 2, z: 4, core: 2. Of those that a mesh axis runs over, the one named last changes fastest.
Arguments:
- residual: bfloat16 [2048, 2048], P(('sp', 'tp')), may hold values from -6 to 6
- ssm_input: bfloat16 [2048, 2048], P('sp', 'tp'), may hold values from -6 to 6
- pole_real: float32 [128, 64], P('tp'), may hold values from -2 to 0
- pole_imaginary: float32 [128, 64], P('tp'), may hold values from 1 to 100
- step_log: float32 [128], P('tp'), may hold values from -8 to 0
- input_real: float32 [128, 64, 16], P('tp'), may hold values from -1 to 1
- entry_map_quadrature: float32 [128, 64, 16], P('tp'), may hold values from -1 to 1
- output_real: float32 [128, 16, 64], P('tp'), may hold values from -0.5 to 0.5
- output_imaginary: float32 [128, 16, 64], P('tp'), may hold values from -0.5 to 0.5
- added_log_decay: float32 [2048, 128], P('sp', 'tp'), may hold values from -2 to 0
- out_weight: bfloat16 [2048, 2048], P('tp'), may hold values from -0.125 to 0.125
- mix_gain: float32 [2048], replicated, may hold values from 0.1 to 1.9
- gate_weight: bfloat16 [2048, 5632], P('sp', 'tp'), may hold values from -0.125 to 0.125
- up_weight: bfloat16 [2048, 5632], P('sp', 'tp'), may hold values from -0.125 to 0.125
- down_weight: bfloat16 [2048, 5632], P('sp', 'tp'), may hold values from -0.078125 to 0.078125
- pre_gain: float32 [2048], replicated, may hold values from 0.1 to 1.9
- post_gain: float32 [2048], replicated, may hold values from 0.1 to 1.9
Outputs:
- merged: bfloat16 [2048, 2048], P(('sp', 'tp'))
The draws below stay inside these ranges and needn't reach their ends.
All inputs are finite; a program needn't handle non-finite values.
Results may differ from the reference program's by a relative error of at most 0.017.
Values may be sent and summed in bfloat16 or wider, within the bound.
A program may use at most 128 MiB of HBM per device.

```python
import math
import jax
import jax.numpy as jnp
from jax import lax

D = 2048
FF = 5632
SSM_WIDTH = 2048
GROUP_CH = 16
STATE = 64
TOK_DEV = 256
CHANNEL_BUNDLES = 128
SEQUENCE_ITEMS = 2048


def frequency_lookup(key):
    base = jax.random.fold_in(key, 11)
    pick_key, slow_key, quick_random_seed, spread_key = jax.random.split(base, 4)
    slow_count = 5
    slow_flag = jax.random.randint(pick_key, (CHANNEL_BUNDLES,), 0, 10) < slow_count
    slow_rate = jnp.exp(jax.random.uniform(slow_key, (CHANNEL_BUNDLES,), jnp.float32, math.log(0.05), math.log(0.5))) / SEQUENCE_ITEMS
    fast_rate = jnp.exp(jax.random.uniform(quick_random_seed, (CHANNEL_BUNDLES,), jnp.float32, math.log(8.0), math.log(16.0))) / TOK_DEV
    rate = jnp.where(slow_flag, slow_rate, fast_rate)
    dispersion = jnp.exp(jax.random.uniform(spread_key, (CHANNEL_BUNDLES, STATE), jnp.float32, -0.3, 0.3))
    return (rate, dispersion)


def draw_pole_real(key, part):
    rate, dispersion = frequency_lookup(key)
    return -jnp.sqrt(rate)[:, None] * dispersion


def draw_step_log(key, part):
    rate, dispersion = frequency_lookup(key)
    return 0.5 * jnp.log(rate)


def draw_added_log_decay(key, part):
    base = jax.random.fold_in(key, 23)
    level_key, where_key, damping_random_seed = jax.random.split(base, 3)
    block_count = SEQUENCE_ITEMS // TOK_DEV
    level = jax.random.uniform(level_key, (block_count, CHANNEL_BUNDLES), jnp.float32, 0.0, 0.4) / SEQUENCE_ITEMS
    baseline_constant = jnp.repeat(level, TOK_DEV, axis=0)
    locations = jax.random.randint(where_key, (2, CHANNEL_BUNDLES), 0, SEQUENCE_ITEMS)
    damping_charges = jax.random.uniform(damping_random_seed, (2, CHANNEL_BUNDLES), jnp.float32, 0.2, 0.4)
    impulse_slots = jnp.arange(SEQUENCE_ITEMS)[:, None, None] == locations[None]
    impulse_tallies = jnp.sum(jnp.where(impulse_slots, jnp.log1p(-damping_charges)[None], 0.0), axis=1)
    return impulse_tallies - baseline_constant


def steps_of(rng, extent, shards, low, high):
    level, own = 1.0, jax.random.fold_in(rng, 6)
    for dim, blocks in shards:
        steps = jnp.exp(jax.random.uniform(jax.random.fold_in(own, dim), (blocks,), jnp.float32, low / len(shards), high / len(shards)))
        level = level * jnp.repeat(steps, extent[dim] // blocks).reshape([-1 if axis == dim else 1 for axis in range(len(extent))])
    return level


def normal_values(own_key, dims, scale, limit, cuts=(), held_as=jnp.bfloat16):
    entries = scale * jax.random.normal(own_key, dims, jnp.float32)
    if cuts:
        entries = entries * steps_of(own_key, dims, cuts, -0.22, 0.18)
    return jnp.clip(entries, -limit, limit).astype(held_as)


def setup_inputs(seed: int = 0) -> dict:
    key_of = jax.random.split(jax.random.key(seed), 18)
    residual = normal_values(key_of[0], (SEQUENCE_ITEMS, D), 1.0, 6.0, ((0, 32),))
    ssm_input = normal_values(key_of[1], (SEQUENCE_ITEMS, SSM_WIDTH), 1.0, 6.0, ((0, 8), (1, 4)))
    pole_real = draw_pole_real(jax.random.fold_in(key_of[17], 71), 0)
    pole_imaginary = jnp.clip(1.0 + 99.0 * jax.random.uniform(key_of[3], (CHANNEL_BUNDLES, STATE), jnp.float32) ** steps_of(key_of[3], (CHANNEL_BUNDLES, STATE), ((0, 4),), -0.2, 0.2), 1.0, 100.0)
    step_log = draw_step_log(jax.random.fold_in(key_of[17], 71), 0)
    input_real = normal_values(key_of[5], (CHANNEL_BUNDLES, STATE, GROUP_CH), (2 * GROUP_CH) ** -0.5, 1.0, ((0, 4),), jnp.float32)
    entry_map_quadrature = normal_values(key_of[6], (CHANNEL_BUNDLES, STATE, GROUP_CH), (2 * GROUP_CH) ** -0.5, 1.0, ((0, 4),), jnp.float32)
    output_real = normal_values(key_of[7], (CHANNEL_BUNDLES, GROUP_CH, STATE), (2 * STATE) ** -0.5, 0.5, ((0, 4),), jnp.float32)
    output_imaginary = normal_values(key_of[8], (CHANNEL_BUNDLES, GROUP_CH, STATE), (2 * STATE) ** -0.5, 0.5, ((0, 4),), jnp.float32)
    added_log_decay = draw_added_log_decay(jax.random.fold_in(key_of[17], 71), 0)
    out_weight = normal_values(key_of[10], (SSM_WIDTH, D), SSM_WIDTH ** -0.5, 0.125, ((0, 4),))
    mix_gain = jnp.clip(1.0 + 0.18 * jax.random.normal(key_of[11], (D,), jnp.float32), 0.1, 1.9)
    gate_weight = normal_values(key_of[12], (D, FF), D ** -0.5, 0.125, ((0, 8), (1, 4)))
    up_weight = normal_values(key_of[13], (D, FF), D ** -0.5, 0.125, ((0, 8), (1, 4)))
    down_weight = normal_values(key_of[14], (D, FF), FF ** -0.5, 0.078125, ((0, 8), (1, 4)))
    pre_gain = jnp.clip(1.0 + 0.18 * jax.random.normal(key_of[15], (D,), jnp.float32), 0.1, 1.9)
    post_gain = jnp.clip(1.0 + 0.18 * jax.random.normal(key_of[16], (D,), jnp.float32), 0.1, 1.9)
    return {"residual": residual, "ssm_input": ssm_input, "pole_real": pole_real, "pole_imaginary": pole_imaginary, "step_log": step_log, "input_real": input_real, "entry_map_quadrature": entry_map_quadrature, "output_real": output_real, "output_imaginary": output_imaginary, "added_log_decay": added_log_decay, "out_weight": out_weight, "mix_gain": mix_gain, "gate_weight": gate_weight, "up_weight": up_weight, "down_weight": down_weight, "pre_gain": pre_gain, "post_gain": post_gain}


EXACT = lax.Precision.HIGHEST
EPSILON = 1e-06

def rms_scale(values, gain):
    return values * lax.rsqrt(lax.optimization_barrier(jnp.mean(values * values, axis=-1, keepdims=True)) + EPSILON) * gain

def round_half(values):
    return lax.optimization_barrier(values.astype(jnp.bfloat16))

def chain_link(earlier, later):
    decay_real, decay_imaginary, state_real, state_imaginary = earlier
    next_real, next_imaginary, drive_real, drive_imaginary = later
    return (next_real * decay_real - next_imaginary * decay_imaginary, next_real * decay_imaginary + next_imaginary * decay_real, next_real * state_real - next_imaginary * state_imaginary + drive_real, next_real * state_imaginary + next_imaginary * state_real + drive_imaginary)

def local_states(inputs, pole_real, pole_imaginary, step_log, input_real, entry_map_quadrature, added_log_decay):
    row_count = inputs.shape[0]
    groups, hidden_states = pole_real.shape
    width = input_real.shape[2]
    step_size = jnp.exp(step_log)[:, None]
    log_size = pole_real * step_size
    angle = pole_imaginary * step_size
    cosine = jnp.cos(angle)
    sine = jnp.sin(angle)
    lift_real = jnp.expm1(log_size) * cosine - 2.0 * jnp.sin(0.5 * angle) ** 2
    lift_imaginary = jnp.exp(log_size) * sine
    denominator = pole_real * pole_real + pole_imaginary * pole_imaginary
    ratio_real = (lift_real * pole_real + lift_imaginary * pole_imaginary) / denominator
    ratio_imaginary = (lift_imaginary * pole_real - lift_real * pole_imaginary) / denominator
    bar_real = ratio_real[..., None] * input_real - ratio_imaginary[..., None] * entry_map_quadrature
    bar_imaginary = ratio_real[..., None] * entry_map_quadrature + ratio_imaginary[..., None] * input_real
    grouped = inputs.astype(jnp.float32).reshape(row_count, groups, width)
    drive_real = jnp.einsum('gnc,tgc->tgn', bar_real, grouped, precision=EXACT).reshape(row_count, groups * hidden_states)
    drive_imaginary = jnp.einsum('gnc,tgc->tgn', bar_imaginary, grouped, precision=EXACT).reshape(row_count, groups * hidden_states)
    pole_magnitude = jnp.exp(log_size[None] + added_log_decay[:, :, None])
    decay_real = (pole_magnitude * cosine[None]).reshape(row_count, groups * hidden_states)
    decay_imaginary = (pole_magnitude * sine[None]).reshape(row_count, groups * hidden_states)
    return lax.associative_scan(chain_link, (decay_real, decay_imaginary, drive_real, drive_imaginary), axis=0)

def apply_carry(scanned, carry_real, carry_imaginary):
    product_real, product_imaginary, state_real, state_imaginary = scanned
    return (state_real + product_real * carry_real - product_imaginary * carry_imaginary, state_imaginary + product_real * carry_imaginary + product_imaginary * carry_real)

def readout(state_real, state_imaginary, output_real, output_imaginary):
    groups, width, hidden_states = output_real.shape
    row_count = state_real.shape[0]
    real_part = jnp.einsum('gcn,tgn->tgc', output_real, state_real.reshape(row_count, groups, hidden_states), precision=EXACT)
    other_part = jnp.einsum('gcn,tgn->tgc', output_imaginary, state_imaginary.reshape(row_count, groups, hidden_states), precision=EXACT)
    return jax.nn.gelu((real_part - other_part).reshape(row_count, groups * width)).astype(jnp.bfloat16)

def reference(residual, ssm_input, pole_real, pole_imaginary, step_log, input_real, entry_map_quadrature, output_real, output_imaginary, added_log_decay, out_weight, mix_gain, gate_weight, up_weight, down_weight, pre_gain, post_gain):
    block_count = SEQUENCE_ITEMS // TOK_DEV

    def per_block(carry, inputs):
        rows_residual, rows_input, rows_extra = inputs
        scanned = local_states(rows_input, pole_real, pole_imaginary, step_log, input_real, entry_map_quadrature, rows_extra)
        state_real, state_imaginary = apply_carry(scanned, carry[0], carry[1])
        activated = readout(state_real, state_imaginary, output_real, output_imaginary)
        mixed = jnp.dot(activated, out_weight, preferred_element_type=jnp.float32)
        middle = round_half(rows_residual.astype(jnp.float32) + rms_scale(mixed, mix_gain))
        mixer_input = rms_scale(middle.astype(jnp.float32), pre_gain).astype(jnp.bfloat16)
        gate_act = jnp.dot(mixer_input, gate_weight, preferred_element_type=jnp.float32)
        up_act = jnp.dot(mixer_input, up_weight, preferred_element_type=jnp.float32)
        hidden = (jax.nn.silu(gate_act) * up_act).astype(jnp.bfloat16)
        mixer_out = lax.dot_general(hidden, down_weight, (((1,), (1,)), ((), ())), preferred_element_type=jnp.float32)
        merged = (middle.astype(jnp.float32) + 0.5 * rms_scale(mixer_out, post_gain)).astype(jnp.bfloat16)
        return ((state_real[-1], state_imaginary[-1]), merged)
    flat_width = pole_real.shape[0] * pole_real.shape[1]
    initial = (jnp.zeros((flat_width,), jnp.float32), jnp.zeros((flat_width,), jnp.float32))
    _, outputs = lax.scan(per_block, initial, (residual.reshape(block_count, TOK_DEV, D), ssm_input.reshape(block_count, TOK_DEV, SSM_WIDTH), added_log_decay.reshape(block_count, TOK_DEV, CHANNEL_BUNDLES)))
    return outputs.reshape(SEQUENCE_ITEMS, D)
```

```python
import functools

import jax
import jax.numpy as jnp
from jax import lax
from jax.experimental import pallas as pl
from jax.experimental.pallas import tpu as pltpu
from jax.sharding import PartitionSpec as P

EPSILON = 1e-06
CHUNKS = 8
LANES = 128
BLOCK = 512
MESH = pl.DeviceIdType.MESH


def rms_scale(values, gain):
    return values * lax.rsqrt(jnp.mean(values * values, axis=-1, keepdims=True) + EPSILON) * gain


def split(values):
    high = values.astype(jnp.bfloat16)
    return high, (values - high.astype(jnp.float32)).astype(jnp.bfloat16)


def dot32(a, b):
    return jnp.dot(a, b, preferred_element_type=jnp.float32)


def times(ar, ai, br, bi):
    return ar * br - ai * bi, ar * bi + ai * br


def greet(barrier, nt):
    place = lax.axis_index("tp")
    for d in range(1, nt):
        pl.semaphore_signal(
            barrier, inc=1, device_id={"tp": lax.rem(place + d, nt)}, device_id_type=MESH
        )


def own_rows(nt, rows):
    own = rows // nt
    return pl.ds(pl.multiple_of(lax.axis_index("tp") * own, own), own)


def scatter_rows(nt, part, landed, sems):
    place = lax.axis_index("tp")
    rows = part.shape[0]
    own = rows // nt
    copies = []
    for d in range(1, nt):
        peer = lax.rem(place + d, nt)
        copy = pltpu.make_async_remote_copy(
            src_ref=part.at[pl.ds(pl.multiple_of(peer * own, own), own)],
            dst_ref=landed.at[d - 1],
            send_sem=sems.at[0, d - 1],
            recv_sem=sems.at[1, d - 1],
            device_id={"tp": peer},
            device_id_type=MESH,
        )
        copy.start()
        copies.append(copy)
    total = part[own_rows(nt, rows), :].astype(jnp.float32)
    for d, copy in enumerate(copies):
        copy.wait()
        total = total + landed[d].astype(jnp.float32)
    return total


def ssm_kernel(
    n,
    nt,
    u,
    mag,
    cr,
    ci,
    er,
    ei,
    rr,
    ri,
    order,
    residual,
    weight,
    mix_gain,
    pre_gain,
    middle,
    out,
    dr,
    di,
    ends,
    send,
    recv,
    start,
    active,
    part,
    landed,
    rows_all,
    send_sem,
    recv_sem,
    tp_sem,
):
    me = lax.axis_index("sp")
    rows, flat = dr.shape
    steps = rows // CHUNKS
    packs, width, wide = er.shape
    block = min(BLOCK, flat)

    barrier = pltpu.get_barrier_semaphore()
    for d in range(1, n):
        pl.semaphore_signal(
            barrier, inc=1, device_id={"sp": lax.rem(me + d, n)}, device_id_type=MESH
        )
    greet(barrier, nt)
    for p in range(packs):
        piece = u[:, p * width : (p + 1) * width]
        for e, dst in ((er, dr), (ei, di)):
            high, low = split(e[p])
            dst[:, p * wide : (p + 1) * wide] = dot32(piece, high) + dot32(piece, low)

    for b in range(0, flat, block):
        at = pl.ds(b, block)
        kr = jnp.broadcast_to(cr[0:1, at], (CHUNKS, block))
        ki = jnp.broadcast_to(ci[0:1, at], (CHUNKS, block))

        def first(j, held):
            pr, pi, sr, si = held
            row = pl.ds(pl.multiple_of(j * CHUNKS, CHUNKS), CHUNKS)
            m = mag[row, at]
            ar, ai = m * kr, m * ki
            pr, pi = times(ar, ai, pr, pi)
            sr, si = times(ar, ai, sr, si)
            return pr, pi, sr + dr[row, at], si + di[row, at]

        zero = jnp.zeros((CHUNKS, block), jnp.float32)
        held = lax.fori_loop(0, steps, first, (zero + 1.0, zero, zero, zero), unroll=2)
        for k in range(4):
            ends[k, :, at] = held[k]

    pr, pi, sr, si = (ends[k, 0:1, :] for k in range(4))
    for c in range(1, CHUNKS):
        ar, ai, br, bi = (ends[k, c : c + 1, :] for k in range(4))
        pr, pi = times(ar, ai, pr, pi)
        sr, si = times(ar, ai, sr, si)
        sr, si = sr + br, si + bi
    for k, item in enumerate((pr, pi, sr, si)):
        send[k : k + 1, :] = item

    pl.semaphore_wait(barrier, n - 1 + nt - 1)
    copies = []
    for d in range(1, n):
        copy = pltpu.make_async_remote_copy(
            src_ref=send,
            dst_ref=recv.at[me],
            send_sem=send_sem.at[d - 1],
            recv_sem=recv_sem.at[d - 1],
            device_id={"sp": lax.rem(me + d, n)},
            device_id_type=MESH,
        )
        copy.start()
        copies.append(copy)
    for copy in copies:
        copy.wait()

    sr = jnp.zeros((1, flat), jnp.float32)
    si = sr
    for k in range(n - 1):
        ar, ai, br, bi = (recv[k, q : q + 1, :] for q in range(4))
        nr, ni = times(ar, ai, sr, si)
        sr = jnp.where(k < me, nr + br, sr)
        si = jnp.where(k < me, ni + bi, si)
    for c in range(CHUNKS):
        start[0, c : c + 1, :] = sr
        start[1, c : c + 1, :] = si
        ar, ai, br, bi = (ends[k, c : c + 1, :] for k in range(4))
        sr, si = times(ar, ai, sr, si)
        sr, si = sr + br, si + bi

    for b in range(0, flat, block):
        at = pl.ds(b, block)
        kr = jnp.broadcast_to(cr[0:1, at], (CHUNKS, block))
        ki = jnp.broadcast_to(ci[0:1, at], (CHUNKS, block))

        def second(j, held):
            row = pl.ds(pl.multiple_of(j * CHUNKS, CHUNKS), CHUNKS)
            m = mag[row, at]
            sr, si = times(m * kr, m * ki, *held)
            sr, si = sr + dr[row, at], si + di[row, at]
            dr[row, at] = sr
            di[row, at] = si
            return sr, si

        lax.fori_loop(0, steps, second, (start[0, :, at], start[1, :, at]), unroll=2)

    for p in range(packs):
        total = None
        for state, read in ((dr, rr), (di, ri)):
            high, low = split(state[:, p * wide : (p + 1) * wide])
            top, rest = split(read[p])
            term = dot32(high, top) + dot32(high, rest) + dot32(low, top)
            total = term if total is None else total + term
        active[:, p * width : (p + 1) * width] = jax.nn.gelu(total).astype(jnp.bfloat16)

    active[...] = dot32(order[...], active[...]).astype(jnp.bfloat16)
    columns = weight.shape[1]
    for b in range(0, columns, BLOCK):
        at = pl.ds(b, BLOCK)
        part[:, at] = dot32(active[...], weight[:, at]).astype(jnp.bfloat16)
    mixed = scatter_rows(nt, part, landed, tp_sem)
    inner = (residual[...].astype(jnp.float32) + rms_scale(mixed, mix_gain[...])).astype(
        jnp.bfloat16
    )
    middle[...] = inner
    own = own_rows(nt, rows)
    rows_all[own, :] = rms_scale(inner.astype(jnp.float32), pre_gain[...]).astype(jnp.bfloat16)
    copies = []
    for d in range(1, nt):
        copy = pltpu.make_async_remote_copy(
            src_ref=rows_all.at[own],
            dst_ref=rows_all.at[own],
            send_sem=tp_sem.at[2, d - 1],
            recv_sem=tp_sem.at[3, d - 1],
            device_id={"tp": lax.rem(lax.axis_index("tp") + d, nt)},
            device_id_type=MESH,
        )
        copy.start()
        copies.append(copy)
    for copy in copies:
        copy.wait()
    out[...] = rows_all[...]


def down_kernel(nt, hidden, weight, middle, gain, out, part, landed, tp_sem):
    barrier = pltpu.get_barrier_semaphore()
    greet(barrier, nt)
    for b in range(0, weight.shape[0], BLOCK):
        at = pl.ds(b, BLOCK)
        part[:, at] = lax.dot_general(
            hidden[...],
            weight[at, :],
            (((1,), (1,)), ((), ())),
            preferred_element_type=jnp.float32,
        ).astype(jnp.bfloat16)
    pl.semaphore_wait(barrier, nt - 1)
    total = scatter_rows(nt, part, landed, tp_sem)
    out[...] = (middle[...].astype(jnp.float32) + 0.5 * rms_scale(total, gain[...])).astype(
        jnp.bfloat16
    )


def branch(
    n,
    nt,
    inputs,
    pole_real,
    pole_imaginary,
    step_log,
    input_real,
    entry_map_quadrature,
    output_real,
    output_imaginary,
    added_log_decay,
    residual,
    out_weight,
    mix_gain,
    pre_gain,
):
    rows, channels = inputs.shape
    columns = out_weight.shape[1]
    groups, states = pole_real.shape
    width = input_real.shape[2]
    flat = groups * states
    step_size = jnp.exp(step_log)[:, None]
    log_size = pole_real * step_size
    angle = pole_imaginary * step_size
    cosine = jnp.cos(angle)
    sine = jnp.sin(angle)
    magnitude = jnp.exp(log_size)
    lift_real = jnp.expm1(log_size) * cosine - 2.0 * jnp.sin(0.5 * angle) ** 2
    lift_imaginary = magnitude * sine
    denominator = pole_real * pole_real + pole_imaginary * pole_imaginary
    ratio_real = (lift_real * pole_real + lift_imaginary * pole_imaginary) / denominator
    ratio_imaginary = (lift_imaginary * pole_real - lift_real * pole_imaginary) / denominator
    bar_real = (
        ratio_real[..., None] * input_real - ratio_imaginary[..., None] * entry_map_quadrature
    )
    bar_imaginary = (
        ratio_real[..., None] * entry_map_quadrature + ratio_imaginary[..., None] * input_real
    )
    pack = LANES // width
    packs = groups // pack
    same = jnp.eye(pack, dtype=jnp.float32)

    def entry(bar):
        bar = bar.reshape(packs, pack, states, width).transpose(0, 1, 3, 2)
        return (bar[:, :, :, None, :] * same[None, :, None, :, None]).reshape(
            packs, pack * width, pack * states
        )

    def read(weight):
        weight = weight.reshape(packs, pack, width, states).transpose(0, 1, 3, 2)
        return (weight[:, :, :, None, :] * same[None, :, None, :, None]).reshape(
            packs, pack * states, pack * width
        )

    def mixed_rows(values):
        return values.reshape(CHUNKS, rows // CHUNKS, -1).transpose(1, 0, 2).reshape(rows, -1)

    spread = jnp.repeat(mixed_rows(jnp.exp(added_log_decay)), states, axis=1)
    vmem = pl.BlockSpec(memory_space=pltpu.VMEM)
    place = jnp.arange(rows)
    order = jax.nn.one_hot(
        place % (rows // CHUNKS) * CHUNKS + place // (rows // CHUNKS), rows, dtype=jnp.bfloat16
    )
    return pl.pallas_call(
        functools.partial(ssm_kernel, n, nt),
        out_shape=(
            jax.ShapeDtypeStruct((rows // nt, columns), jnp.bfloat16),
            jax.ShapeDtypeStruct((rows, columns), jnp.bfloat16),
        ),
        in_specs=[vmem] * 13,
        out_specs=(vmem, vmem),
        scratch_shapes=[
            pltpu.VMEM((rows, flat), jnp.float32),
            pltpu.VMEM((rows, flat), jnp.float32),
            pltpu.VMEM((4, CHUNKS, flat), jnp.float32),
            pltpu.VMEM((CHUNKS, flat), jnp.float32),
            pltpu.VMEM((n, CHUNKS, flat), jnp.float32),
            pltpu.VMEM((2, CHUNKS, flat), jnp.float32),
            pltpu.VMEM((rows, channels), jnp.bfloat16),
            pltpu.VMEM((rows, columns), jnp.bfloat16),
            pltpu.VMEM((nt - 1, rows // nt, columns), jnp.bfloat16),
            pltpu.VMEM((rows, columns), jnp.bfloat16),
            pltpu.SemaphoreType.DMA((n - 1,)),
            pltpu.SemaphoreType.DMA((n - 1,)),
            pltpu.SemaphoreType.DMA((4, nt - 1)),
        ],
        cost_estimate=pl.CostEstimate(
            flops=24000000000, bytes_accessed=8000000, transcendentals=0
        ),
        compiler_params=pltpu.CompilerParams(
            collective_id=0, has_side_effects=True, vmem_limit_bytes=40 * 1024 * 1024
        ),
    )(
        mixed_rows(inputs),
        spread,
        (magnitude * cosine).reshape(1, flat),
        (magnitude * sine).reshape(1, flat),
        entry(bar_real),
        entry(bar_imaginary),
        read(output_real),
        read(-output_imaginary),
        order,
        residual,
        out_weight,
        mix_gain.reshape(1, columns),
        pre_gain.reshape(1, columns),
    )


def shards(
    n,
    nt,
    residual,
    ssm_input,
    pole_real,
    pole_imaginary,
    step_log,
    input_real,
    entry_map_quadrature,
    output_real,
    output_imaginary,
    added_log_decay,
    out_weight,
    mix_gain,
    gate_weight,
    up_weight,
    down_weight,
    pre_gain,
    post_gain,
):
    gate_full, up_full, down_full = (
        lax.all_gather(gate_weight, "sp", axis=0, tiled=True),
        lax.all_gather(up_weight, "sp", axis=0, tiled=True),
        lax.all_gather(down_weight, "sp", axis=0, tiled=True),
    )
    middle, mixer_input = branch(
        n,
        nt,
        ssm_input,
        pole_real,
        pole_imaginary,
        step_log,
        input_real,
        entry_map_quadrature,
        output_real,
        output_imaginary,
        added_log_decay,
        residual,
        out_weight,
        mix_gain,
        pre_gain,
    )
    gate_act = jnp.dot(mixer_input, gate_full, preferred_element_type=jnp.float32)
    up_act = jnp.dot(mixer_input, up_full, preferred_element_type=jnp.float32)
    hidden = (jax.nn.silu(gate_act) * up_act).astype(jnp.bfloat16)
    rows, columns = mixer_input.shape
    return pl.pallas_call(
        functools.partial(down_kernel, nt),
        out_shape=jax.ShapeDtypeStruct(residual.shape, jnp.bfloat16),
        in_specs=[pl.BlockSpec(memory_space=pltpu.VMEM)] * 4,
        out_specs=pl.BlockSpec(memory_space=pltpu.VMEM),
        scratch_shapes=[
            pltpu.VMEM((rows, columns), jnp.bfloat16),
            pltpu.VMEM((nt - 1, rows // nt, columns), jnp.bfloat16),
            pltpu.SemaphoreType.DMA((2, nt - 1)),
        ],
        cost_estimate=pl.CostEstimate(flops=8000000000, bytes_accessed=8000000, transcendentals=0),
        compiler_params=pltpu.CompilerParams(
            collective_id=1, has_side_effects=True, vmem_limit_bytes=24 * 1024 * 1024
        ),
    )(hidden, down_full, middle, post_gain.reshape(1, columns))


def solution(mesh):
    return jax.shard_map(
        functools.partial(shards, mesh.shape["sp"], mesh.shape["tp"]),
        mesh=mesh,
        in_specs=(
            P(("sp", "tp"), None),
            P("sp", "tp"),
            P("tp", None),
            P("tp", None),
            P("tp"),
            P("tp", None, None),
            P("tp", None, None),
            P("tp", None, None),
            P("tp", None, None),
            P("sp", "tp"),
            P("tp", None),
            P(),
            P("sp", "tp"),
            P("sp", "tp"),
            P("sp", "tp"),
            P(),
            P(),
        ),
        out_specs=P(("sp", "tp"), None),
        check_vma=False,
    )
```
